32 devices in a mesh: ep: 16 (over z, y, x), tp: 2 (over core).
Axes of the slice: x: 2, y: 2, z: 4, core: 2. Of those that a mesh axis runs over, the one named last changes fastest.
Arguments:
- tokens: bfloat16 [512, 4096], P('ep'), may hold values from -6 to 6
- norm_gain: float32 [4096], replicated, may hold values from 0.1 to 1.9
- expert_ids: int32 [512, 2], P('ep'), may hold values from 0 to 15, all different within a row; in each aligned block of 32 rows (0 to 31, 32 to 63, ...) at most 8 rows name the same one
- gates: float32 [512, 2], P('ep'), may hold values from 0.1 to 1
- w_gate: bfloat16 [16, 4096, 768], P('ep', None, 'tp'), may hold values from -0.09375 to 0.09375
- w_up: bfloat16 [16, 4096, 768], P('ep', None, 'tp'), may hold values from -0.09375 to 0.09375
- w_down: bfloat16 [16, 768, 4096], P('ep', 'tp'), may hold values from -1 to 1, as said below
- post_gain: float32 [4096], P('tp'), may hold values from 0.1 to 1.9
Outputs:
- mixed: bfloat16 [512, 4096], P('ep', 'tp')
The draws below stay inside these ranges and needn't reach their ends.
Inputs may be any that keep to these rules, and one draw needn't show every extreme that they name: `expert_ids`: each row names 2 different experts; among the 32 rows of one device (aligned blocks) no expert is named more than 8 times. `w_down`: entries of the down projections lie between -1 and 1, both reached.
All inputs are finite; a program needn't handle non-finite values.
Results may differ from the reference program's by a relative error of at most 0.015.
Values may be sent and summed in bfloat16 or wider, within the bound.
A program may use at most 64 MiB of HBM per device.

```python
import math
import jax
import jax.numpy as jnp
import numpy as np
from jax import lax

D = 4096
FF = 768
TOP_K = 2
TOK_DEV = 32
SLOTS = 8
TOKENS = 512
EXPERTS = 16
N_EP = 16


def draw_w_down(key, part):
    scale_key = jax.random.fold_in(key, 11)
    value_key = jax.random.fold_in(key, 23)
    log_scale = jax.random.uniform(scale_key, (EXPERTS, 1, 1), jnp.float32, -1.0986, 1.0986)
    factor = jnp.exp(log_scale)
    column = jnp.arange(D, dtype=jnp.int32)[None, None, :]
    column_scale = jnp.where(column < D // 2, factor, 1.0 / factor)
    base = jnp.clip(jax.random.normal(value_key, (EXPERTS, FF, D), jnp.float32), -5.0, 5.0)
    values = base * column_scale * FF ** (-0.5)
    values = jnp.clip(values, -1.0, 1.0)
    values = values.at[0, 0, 0].set(1.0)
    values = values.at[0, 0, 1].set(-1.0)
    return values.astype(jnp.bfloat16)


def steps_of(own_key, dims, shards, least, high):
    def one(position, shards_of):
        steps = jax.random.uniform(jax.random.fold_in(jax.random.fold_in(own_key, 6), position), (shards_of,), jnp.float32, least / len(shards), high / len(shards))
        return jnp.repeat(jnp.exp(steps), dims[position] // shards_of).reshape((-1,) + (1,) * (len(dims) - position - 1))

    factor_of = one(*shards[0])
    for cut in shards[1:]:
        factor_of = factor_of * one(*cut)
    return factor_of


def shared_out(stream_key, own, number, rows, amount, top, reach, lean):
    order = jax.random.permutation(stream_key, amount)
    heavy_load, usual = portions_of(amount, rows * top, reach, lean, True), portions_of(amount, rows * top, reach, lean, False)
    places = jnp.arange(amount)

    def named(lengths, turn):
        used = int((lengths > 0).sum())
        fixed = max(1, used // 4)
        passed = fixed + (places - fixed + turn * (used - fixed)) % max(1, amount - fixed)
        return jnp.zeros((amount,), jnp.int32).at[order[jnp.where(places < fixed, places, passed)]].set(jnp.asarray(lengths, jnp.int32))

    lengths = jnp.where(number % 4 == 0, named(heavy_load, number // 4), named(usual, number - number // 4 - 1))
    mixed = jax.random.permutation(jax.random.fold_in(own, 3), amount)
    giver, taker = mixed[0:amount // 2 * 2:2], mixed[1:amount // 2 * 2:2]
    slack = jnp.minimum(lengths[giver] - 1, reach - lengths[taker]) // 2
    slack = jnp.where((giver == order[0]) | (taker == order[0]) | (lengths[taker] == 0), 0, jnp.maximum(slack, 0))
    passed = jax.random.randint(jax.random.fold_in(own, 4), (amount // 2,), 0, 1 << 20) % (slack + 1)
    lengths = lengths.at[giver].add(-passed).at[taker].add(passed)
    members = jnp.searchsorted(jnp.cumsum(lengths), jnp.arange(rows * top), side="right").astype(jnp.int32)
    grid = members.reshape(top, rows).T
    grid = grid[jax.random.permutation(jax.random.fold_in(own, 1), rows)]
    turn = jax.random.randint(jax.random.fold_in(own, 2), (rows, 1), 0, top)
    return jnp.take_along_axis(grid, (jnp.arange(top)[None, :] + turn) % top, axis=1)


def portions_of(count, total, reach, lean, full):
    portions = [(1 << 20) // math.isqrt(standing ** lean) + 1 for standing in range(1, count + 1)]
    largest = reach if full else min(reach, max(-(-total // count), total * portions[0] // sum(portions)))
    least = 1 if total - largest >= count - 1 else 0
    counts, spare = [largest] + [least] * (count - 1), total - largest - least * (count - 1)
    while spare > 0:
        candidates = [i for i in range(1, count) if counts[i] < largest] or [i for i in range(1, count) if counts[i] < reach]
        pool, budget = sum([portions[i] for i in candidates]), spare
        for i in candidates:
            addition = min(reach - counts[i], max(1, budget * portions[i] // pool), spare)
            counts[i] = counts[i] + addition
            spare = spare - addition
    return np.array(counts)


def bell_draw(rng, shape, scale, bound, pieces=(), kind=jnp.bfloat16):
    level = steps_of(rng, shape, pieces, -0.22, 0.18) if pieces else 1.0
    array = jax.random.normal(rng, shape, jnp.float32) * scale * level
    return jnp.minimum(jnp.maximum(array, -bound), bound).astype(kind)


def setup_inputs(seed: int = 0) -> dict:
    key_list = jax.random.split(jax.random.key(seed), 9)
    tokens = bell_draw(key_list[0], (TOKENS, D), 1.0, 6.0, ((0, 16),))
    norm_gain = jnp.clip(1.0 + 0.18 * jax.random.normal(key_list[1], (D,), jnp.float32), 0.1, 1.9)
    expert_ids_keys = jax.random.split(jax.random.fold_in(key_list[2], 1), TOKENS // TOK_DEV)
    expert_ids_turns = jax.random.permutation(jax.random.fold_in(key_list[2], 3), TOKENS // TOK_DEV)
    expert_ids = jax.vmap(lambda own, number: shared_out(jax.random.fold_in(key_list[2], 2), own, number, TOK_DEV, EXPERTS, TOP_K, SLOTS, 2))(expert_ids_keys, expert_ids_turns).reshape((TOKENS, TOP_K))
    gates = jnp.clip(0.1 + 0.9 * jax.random.uniform(key_list[3], (TOKENS, TOP_K), jnp.float32) ** steps_of(key_list[3], (TOKENS, TOP_K), ((0, 16),), -0.2, 0.2), 0.1, 1.0)
    w_gate = bell_draw(key_list[4], (EXPERTS, D, FF), D ** -0.5, 0.09375, ((0, 16), (2, 2)))
    w_up = bell_draw(key_list[5], (EXPERTS, D, FF), D ** -0.5, 0.09375, ((0, 16), (2, 2)))
    w_down = draw_w_down(jax.random.fold_in(key_list[8], 71), 0)
    post_gain = jnp.clip(1.0 + 0.18 * jax.random.normal(key_list[7], (D,), jnp.float32), 0.1, 1.9)
    return {"tokens": tokens, "norm_gain": norm_gain, "expert_ids": expert_ids, "gates": gates, "w_gate": w_gate, "w_up": w_up, "w_down": w_down, "post_gain": post_gain}


RMS_EPS = 1e-06

def rms_scale(values, gain):
    floats = values.astype(jnp.float32)
    inverse = lax.rsqrt(lax.optimization_barrier(jnp.mean(floats * floats, axis=-1, keepdims=True)) + RMS_EPS)
    return (floats * inverse * gain).astype(jnp.bfloat16)

def reference(tokens, norm_gain, expert_ids, gates, w_gate, w_up, w_down, post_gain):
    normed = rms_scale(tokens, norm_gain)
    capacity = N_EP * SLOTS
    flat_ids = expert_ids.reshape(-1)
    flat_gates = gates.reshape(-1)
    route_total = TOKENS * TOP_K
    route_index = jnp.arange(route_total, dtype=jnp.int32)

    def step_one(carry, inputs):
        expert_num, gate_mat, up_mat, down_mat = inputs
        to_mine = flat_ids == expert_num
        rank = jnp.cumsum(to_mine.astype(jnp.int32)) - 1
        slot_target = jnp.where(to_mine, rank, capacity).astype(jnp.int32)
        slot_route = jnp.zeros((capacity,), jnp.int32).at[slot_target].set(route_index, mode='drop')
        filled = jnp.zeros((capacity,), jnp.float32).at[slot_target].set(1.0, mode='drop')
        token_of = (slot_route // TOP_K).astype(jnp.int32)
        picked_rows = jnp.where(filled[:, None] > 0, normed[token_of], jnp.zeros((), jnp.bfloat16))
        gate_proj = jnp.dot(picked_rows, gate_mat, preferred_element_type=jnp.float32)
        up_proj = jnp.dot(picked_rows, up_mat, preferred_element_type=jnp.float32)
        hidden = (jax.nn.silu(gate_proj) * up_proj).astype(jnp.bfloat16)
        expert_out = jnp.dot(hidden, down_mat, preferred_element_type=jnp.float32).astype(jnp.bfloat16)
        weights = flat_gates[slot_route] * filled
        carry = carry.at[token_of].add(expert_out.astype(jnp.float32) * weights[:, None])
        return (carry, None)
    start = jnp.zeros((TOKENS, D), jnp.float32)
    combined, _ = lax.scan(step_one, start, (jnp.arange(EXPERTS, dtype=jnp.int32), w_gate, w_up, w_down))
    return rms_scale(combined.astype(jnp.bfloat16), post_gain)
```

```python
import functools

import jax
import jax.numpy as jnp
from jax import lax
from jax.experimental import pallas as pl
from jax.experimental.pallas import tpu as pltpu
from jax.sharding import PartitionSpec as P

SLOTS = 8
RMS_EPS = 1e-06
MESH = pl.DeviceIdType.MESH
F32 = jnp.float32
BF16 = jnp.bfloat16


def kernel(
    n, n_tp,
    tok_ref, gain_ref, ids_ref, gates_ref, post_ref, wg_ref, wu_ref, wd_ref,
    out_ref,
    send_buf, x_buf, wgu, wdn, h_buf, o_buf, ret_buf, stat_buf,
    w_sem, wx_send, wx_recv, d_send, d_recv, f_send, f_recv,
    h_send, h_recv, r_send, r_recv, s_send, s_recv,
):
    me = lax.axis_index("ep")
    core = lax.axis_index("tp")
    other = 1 - core
    rows, features = tok_ref.shape
    half = features // n_tp
    part = wg_ref.shape[2]
    cap = n * SLOTS

    def step(i):
        return 1 + lax.rem(n // 2 - 1 + i, n - 1)

    barrier = pltpu.get_barrier_semaphore()

    def greet(k, _):
        pl.semaphore_signal(barrier, inc=1, device_id={"ep": lax.rem(me + k, n)}, device_id_type=MESH)
        return 0

    lax.fori_loop(1, n, greet, 0)
    pl.semaphore_signal(barrier, inc=1, device_id={"tp": other}, device_id_type=MESH)

    own_cols = pl.ds(pl.multiple_of(core * half, half), half)
    other_cols = pl.ds(pl.multiple_of(other * half, half), half)
    own_part = pl.ds(pl.multiple_of(core * part, part), part)
    copies = [
        pltpu.make_async_copy(wg_ref.at[0], wgu.at[:, pl.ds(0, part)], w_sem.at[0]),
        pltpu.make_async_copy(wu_ref.at[0], wgu.at[:, pl.ds(part, part)], w_sem.at[1]),
        pltpu.make_async_copy(wd_ref.at[0, :, own_cols], wdn.at[own_part], w_sem.at[2]),
    ]
    for copy in copies:
        copy.start()

    ids = ids_ref[...]
    lanes = lax.broadcasted_iota(jnp.int32, (rows, n), 1)
    before = (
        lax.broadcasted_iota(jnp.int32, (rows, rows), 1)
        < lax.broadcasted_iota(jnp.int32, (rows, rows), 0)
    ).astype(BF16)
    slots = lax.broadcasted_iota(jnp.int32, (rows, cap), 1)
    count = jnp.zeros((1, n), F32)
    picks = []
    for j in range(ids.shape[1]):
        hot = (ids[:, j:j + 1] == lanes).astype(F32)
        earlier = jnp.dot(before, hot.astype(BF16), preferred_element_type=F32) + count
        slot = jnp.sum(earlier * hot, axis=1, keepdims=True).astype(jnp.int32)
        count = count + jnp.sum(hot, axis=0, keepdims=True)
        picks.append((slots == ids[:, j:j + 1] * SLOTS + slot).astype(F32))

    floats = tok_ref[...].astype(F32)
    inverse = lax.rsqrt(jnp.mean(floats * floats, axis=1, keepdims=True) + RMS_EPS)
    mine = tok_ref[:, own_cols].astype(F32)
    normed = (mine * inverse * gain_ref[:, own_cols]).astype(BF16)
    dispatch = functools.reduce(lambda a, b: a + b, picks).T.astype(BF16)
    sent = jnp.dot(dispatch, normed, preferred_element_type=F32)
    send_buf[...] = sent.reshape(n, SLOTS, half).astype(BF16)

    pl.semaphore_wait(barrier, n)

    def to_expert(i):
        peer = lax.rem(me + step(i), n)
        return pltpu.make_async_remote_copy(
            src_ref=send_buf.at[peer], dst_ref=x_buf.at[me, core],
            send_sem=d_send.at[peer], recv_sem=d_recv.at[me],
            device_id={"ep": peer}, device_id_type=MESH)

    def from_token(i):
        peer = lax.rem(me + n - step(i), n)
        return peer, pltpu.make_async_remote_copy(
            src_ref=send_buf.at[peer], dst_ref=x_buf.at[peer, core],
            send_sem=d_send.at[peer], recv_sem=d_recv.at[peer],
            device_id={"ep": peer}, device_id_type=MESH)

    def forward(src, block):
        return pltpu.make_async_remote_copy(
            src_ref=src, dst_ref=x_buf.at[block, core],
            send_sem=f_send.at[block], recv_sem=f_recv.at[block],
            device_id={"tp": other}, device_id_type=MESH)

    def start_send(i, _):
        to_expert(i).start()
        return 0

    lax.fori_loop(0, n - 1, start_send, 0)
    own_x = pltpu.make_async_copy(send_buf.at[me], x_buf.at[me, core], w_sem.at[3])
    own_x.start()
    forward(send_buf.at[me], me).start()
    down_x = pltpu.make_async_remote_copy(
        src_ref=wd_ref.at[0, :, other_cols], dst_ref=wdn.at[own_part],
        send_sem=wx_send, recv_sem=wx_recv,
        device_id={"tp": other}, device_id_type=MESH)
    down_x.start()

    def pass_on(i, _):
        peer, copy = from_token(i)
        copy.wait_recv()
        forward(x_buf.at[peer, core], peer).start()
        return 0

    lax.fori_loop(0, n - 1, pass_on, 0)
    own_x.wait()

    def arrived(i, _):
        forward(x_buf.at[i, core], i).wait_recv()
        return 0

    lax.fori_loop(0, n, arrived, 0)
    for copy in copies:
        copy.wait()

    acc = jnp.zeros((cap, 2 * part), F32)
    for side in range(n_tp):
        x = x_buf[:, side].astype(F32).reshape(cap, half).astype(BF16)
        acc = acc + jnp.dot(x, wgu[side * half:(side + 1) * half], preferred_element_type=F32)
    gate = acc[:, :part]
    up = acc[:, part:]
    hidden = (gate / (1.0 + jnp.exp(-gate)) * up).astype(BF16)
    h_buf[:, own_part] = hidden
    hx = pltpu.make_async_remote_copy(
        src_ref=h_buf.at[:, own_part], dst_ref=h_buf.at[:, own_part],
        send_sem=h_send, recv_sem=h_recv,
        device_id={"tp": other}, device_id_type=MESH)
    hx.start()
    down_x.wait()
    hx.wait()

    result = jnp.dot(h_buf[...], wdn[...], preferred_element_type=F32)
    o_buf[...] = result.reshape(n, SLOTS, half).astype(BF16)

    def give_back(i):
        peer = lax.rem(me + step(i), n)
        return pltpu.make_async_remote_copy(
            src_ref=o_buf.at[peer], dst_ref=ret_buf.at[me],
            send_sem=r_send.at[peer], recv_sem=r_recv.at[me],
            device_id={"ep": peer}, device_id_type=MESH)

    def take_back(i):
        peer = lax.rem(me + n - step(i), n)
        return pltpu.make_async_remote_copy(
            src_ref=o_buf.at[peer], dst_ref=ret_buf.at[peer],
            send_sem=r_send.at[peer], recv_sem=r_recv.at[peer],
            device_id={"ep": peer}, device_id_type=MESH)

    def start_back(i, _):
        give_back(i).start()
        return 0

    lax.fori_loop(0, n - 1, start_back, 0)
    own_r = pltpu.make_async_copy(o_buf.at[me], ret_buf.at[me], w_sem.at[4])
    own_r.start()

    def sent_all(i, _):
        to_expert(i).wait_send()
        return 0

    lax.fori_loop(0, n - 1, sent_all, 0)

    def passed_all(i, _):
        forward(x_buf.at[i, core], i).wait_send()
        return 0

    lax.fori_loop(0, n, passed_all, 0)

    def back(i, _):
        take_back(i).wait_recv()
        return 0

    lax.fori_loop(0, n - 1, back, 0)
    own_r.wait()

    returned = ret_buf[...].astype(F32).reshape(cap, half).astype(BF16)
    combined = jnp.zeros((rows, half), F32)
    for j, pick in enumerate(picks):
        row = jnp.dot(pick.astype(BF16), returned, preferred_element_type=F32)
        combined = combined + gates_ref[:, j:j + 1] * row
    low = combined.astype(BF16).astype(F32)
    squared = jnp.sum(low * low, axis=1, keepdims=True)
    stat_buf[0] = jnp.broadcast_to(squared, (rows, 128))
    sx = pltpu.make_async_remote_copy(
        src_ref=stat_buf.at[0], dst_ref=stat_buf.at[1],
        send_sem=s_send, recv_sem=s_recv,
        device_id={"tp": other}, device_id_type=MESH)
    sx.start()

    def back_sent(i, _):
        give_back(i).wait_send()
        return 0

    lax.fori_loop(0, n - 1, back_sent, 0)
    sx.wait()
    total = squared + stat_buf[1][:, 0:1]
    scale = lax.rsqrt(total / features + RMS_EPS)
    out_ref[...] = (low * scale * post_ref[...]).astype(BF16)


def shards(n, n_tp, tokens, norm_gain, expert_ids, gates, w_gate, w_up, w_down, post_gain):
    rows, features = tokens.shape
    half = features // n_tp
    part = w_gate.shape[2]
    vmem = pl.BlockSpec(memory_space=pltpu.VMEM)
    hbm = pl.BlockSpec(memory_space=pl.ANY)
    dma = pltpu.SemaphoreType.DMA
    cap = n * SLOTS
    return pl.pallas_call(
        functools.partial(kernel, n, n_tp),
        out_shape=jax.ShapeDtypeStruct((rows, half), BF16),
        in_specs=[vmem] * 5 + [hbm] * 3,
        out_specs=vmem,
        scratch_shapes=[
            pltpu.VMEM((n, SLOTS, half), BF16),
            pltpu.VMEM((n, n_tp, SLOTS, half), BF16),
            pltpu.VMEM((features, 2 * part), BF16),
            pltpu.VMEM((n_tp * part, half), BF16),
            pltpu.VMEM((cap, n_tp * part), BF16),
            pltpu.VMEM((n, SLOTS, half), BF16),
            pltpu.VMEM((n, SLOTS, half), BF16),
            pltpu.VMEM((2, rows, 128), F32),
            dma((5,)), dma, dma,
            dma((n,)), dma((n,)), dma((n,)), dma((n,)),
            dma, dma, dma((n,)), dma((n,)), dma, dma,
        ],
        compiler_params=pltpu.CompilerParams(
            collective_id=0, has_side_effects=True, vmem_limit_bytes=60 * 1024 * 1024
        ),
    )(
        tokens, norm_gain.reshape(1, -1), expert_ids, gates, post_gain.reshape(1, -1),
        w_gate, w_up, w_down,
    )


def solution(mesh):
    in_specs = (
        P("ep", None),
        P(),
        P("ep", None),
        P("ep", None),
        P("ep", None, "tp"),
        P("ep", None, "tp"),
        P("ep", "tp", None),
        P("tp"),
    )
    body = functools.partial(shards, mesh.shape["ep"], mesh.shape["tp"])
    return jax.shard_map(body, mesh=mesh, in_specs=in_specs, out_specs=P("ep", "tp"), check_vma=False)
```

```python
import functools

import jax
import jax.numpy as jnp
from jax import lax
from jax.experimental import pallas as pl
from jax.experimental.pallas import tpu as pltpu
from jax.sharding import PartitionSpec as P

SLOTS = 8
RMS_EPS = 1e-06
MESH = pl.DeviceIdType.MESH
F32 = jnp.float32
BF16 = jnp.bfloat16


def kernel(
    n, n_tp,
    tok_ref, gain_ref, ids_ref, gates_ref, post_ref, wg_ref, wu_ref, wd_ref,
    out_ref,
    send_buf, x_buf, wgu, wdn, h_buf, o_buf, ret_buf, stat_buf,
    w_sem, wx_send, wx_recv, d_send, d_recv, f_send, f_recv,
    h_send, h_recv, r_send, r_recv, s_send, s_recv,
):
    me = lax.axis_index("ep")
    core = lax.axis_index("tp")
    other = 1 - core
    rows, features = tok_ref.shape
    half = features // n_tp
    part = wg_ref.shape[2]
    cap = n * SLOTS

    groups = 4 if n % 4 == 0 else 1
    order = (2, 0, 3, 1) if groups == 4 else (0,)
    wide = n // groups
    plane, place = me // wide, lax.rem(me, wide)

    def target(q, r):
        return lax.rem(plane + order[q], groups) * wide + lax.rem(place + r, wide)

    def origin(q, r):
        return lax.rem(plane + groups - order[q], groups) * wide + lax.rem(place + wide - r, wide)

    def each(q, body):
        def go(r, _):
            body(q, r, q * wide + r)
            return 0

        lax.fori_loop(0 if order[q] else 1, wide, go, 0)

    own = order.index(0) * wide

    barrier = pltpu.get_barrier_semaphore()

    def greet(k, _):
        pl.semaphore_signal(barrier, inc=1, device_id={"ep": lax.rem(me + k, n)}, device_id_type=MESH)
        return 0

    lax.fori_loop(1, n, greet, 0)
    pl.semaphore_signal(barrier, inc=1, device_id={"tp": other}, device_id_type=MESH)

    own_cols = pl.ds(pl.multiple_of(core * half, half), half)
    other_cols = pl.ds(pl.multiple_of(other * half, half), half)
    own_part = pl.ds(pl.multiple_of(core * part, part), part)
    copies = [
        pltpu.make_async_copy(wg_ref.at[0], wgu.at[:, pl.ds(0, part)], w_sem.at[0]),
        pltpu.make_async_copy(wu_ref.at[0], wgu.at[:, pl.ds(part, part)], w_sem.at[1]),
        pltpu.make_async_copy(wd_ref.at[0, :, own_cols], wdn.at[own_part], w_sem.at[2]),
    ]
    for copy in copies:
        copy.start()

    ids = ids_ref[...]
    names = lax.broadcasted_iota(jnp.int32, (n, rows), 0)
    first = lax.broadcasted_iota(jnp.int32, (rows, rows), 0)
    second = lax.broadcasted_iota(jnp.int32, (rows, rows), 1)
    before = (first < second).astype(BF16)
    same = first == second
    slots = lax.broadcasted_iota(jnp.int32, (cap, rows), 0)
    count = jnp.zeros((n, 1), F32)
    picks = []
    for j in range(ids.shape[0]):
        hot = (ids[j:j + 1] == names).astype(F32)
        earlier = jnp.dot(hot.astype(BF16), before, preferred_element_type=F32) + count
        slot = jnp.sum(earlier * hot, axis=0, keepdims=True).astype(jnp.int32)
        count = count + jnp.sum(hot, axis=1, keepdims=True)
        picks.append((slots == ids[j:j + 1] * SLOTS + slot).astype(F32))

    floats = tok_ref[...].astype(F32)
    inverse = lax.rsqrt(jnp.mean(floats * floats, axis=1, keepdims=True) + RMS_EPS)
    mine = tok_ref[:, own_cols].astype(F32)
    normed = (mine * inverse * gain_ref[:, own_cols]).astype(BF16)
    dispatch = functools.reduce(lambda a, b: a + b, picks).astype(BF16)
    sent = jnp.dot(dispatch, normed, preferred_element_type=F32)
    send_buf[...] = sent.reshape(n, SLOTS, half).astype(BF16)

    pl.semaphore_wait(barrier, n)

    def to_expert(q, r, i):
        peer = target(q, r)
        return pltpu.make_async_remote_copy(
            src_ref=send_buf.at[peer], dst_ref=x_buf.at[i, core],
            send_sem=d_send.at[i], recv_sem=d_recv.at[i],
            device_id={"ep": peer}, device_id_type=MESH)

    def forward(src, block):
        return pltpu.make_async_remote_copy(
            src_ref=src, dst_ref=x_buf.at[block, core],
            send_sem=f_send.at[block], recv_sem=f_recv.at[block],
            device_id={"tp": other}, device_id_type=MESH)

    for q in range(groups):
        each(q, lambda q, r, i: to_expert(q, r, i).start())
    own_x = pltpu.make_async_copy(send_buf.at[me], x_buf.at[own, core], w_sem.at[3])
    own_x.start()
    forward(send_buf.at[me], own).start()
    down_x = pltpu.make_async_remote_copy(
        src_ref=wd_ref.at[0, :, other_cols], dst_ref=wdn.at[own_part],
        send_sem=wx_send, recv_sem=wx_recv,
        device_id={"tp": other}, device_id_type=MESH)
    down_x.start()
    own_r = pltpu.make_async_copy(o_buf.at[own], ret_buf.at[me], w_sem.at[4])

    def pass_on(q, r, i):
        to_expert(q, r, i).wait_recv()
        forward(x_buf.at[i, core], i).start()

    def give_back(q, r, i):
        peer = origin(q, r)
        return pltpu.make_async_remote_copy(
            src_ref=o_buf.at[i], dst_ref=ret_buf.at[me],
            send_sem=r_send.at[i], recv_sem=r_recv.at[me],
            device_id={"ep": peer}, device_id_type=MESH)

    def take_back(q, r, i):
        peer = target(q, r)
        return pltpu.make_async_remote_copy(
            src_ref=o_buf.at[i], dst_ref=ret_buf.at[peer],
            send_sem=r_send.at[i], recv_sem=r_recv.at[peer],
            device_id={"ep": peer}, device_id_type=MESH)

    span = max(groups // 2, 1)
    for chunk in range(groups // span):
        mine_q = range(chunk * span, (chunk + 1) * span)
        start, size = chunk * span * wide, span * wide
        for q in mine_q:
            each(q, pass_on)
        if start <= own < start + size:
            own_x.wait()

        def arrived(i, _):
            forward(x_buf.at[i, core], i).wait_recv()
            return 0

        lax.fori_loop(start, start + size, arrived, 0)
        if chunk == 0:
            for copy in copies:
                copy.wait()
        acc = jnp.zeros((size * SLOTS, 2 * part), F32)
        for side in range(n_tp):
            x = x_buf[start:start + size, side].astype(F32).reshape(size * SLOTS, half).astype(BF16)
            acc = acc + jnp.dot(x, wgu[side * half:(side + 1) * half], preferred_element_type=F32)
        gate = acc[:, :part]
        up = acc[:, part:]
        hidden = (gate / (1.0 + jnp.exp(-gate)) * up).astype(BF16)
        lines = pl.ds(start * SLOTS, size * SLOTS)
        h_buf[lines, own_part] = hidden
        hx = pltpu.make_async_remote_copy(
            src_ref=h_buf.at[lines, own_part], dst_ref=h_buf.at[lines, own_part],
            send_sem=h_send.at[chunk], recv_sem=h_recv.at[chunk],
            device_id={"tp": other}, device_id_type=MESH)
        hx.start()
        if chunk == 0:
            down_x.wait()
        hx.wait()
        result = jnp.dot(h_buf[lines], wdn[...], preferred_element_type=F32)
        o_buf[start:start + size] = result.reshape(size, SLOTS, half).astype(BF16)
        for q in mine_q:
            each(q, lambda q, r, i: give_back(q, r, i).start())
        if start <= own < start + size:
            own_r.start()

    for q in range(groups):
        each(q, lambda q, r, i: to_expert(q, r, i).wait_send())

    def passed_all(i, _):
        forward(x_buf.at[i, core], i).wait_send()
        return 0

    lax.fori_loop(0, n, passed_all, 0)
    gates = [
        jnp.sum(jnp.where(same, gates_ref[j:j + 1], 0.0), axis=1, keepdims=True)
        for j in range(ids.shape[0])
    ]
    picks = [pick.T.astype(BF16) for pick in picks]
    for q in range(groups):
        each(q, lambda q, r, i: take_back(q, r, i).wait_recv())
    own_r.wait()

    returned = ret_buf[...].astype(F32).reshape(cap, half).astype(BF16)
    combined = jnp.zeros((rows, half), F32)
    for j, pick in enumerate(picks):
        row = jnp.dot(pick, returned, preferred_element_type=F32)
        combined = combined + gates[j] * row
    low = combined.astype(BF16).astype(F32)
    squared = jnp.sum(low * low, axis=1, keepdims=True)
    stat_buf[0] = jnp.broadcast_to(squared, (rows, 128))
    sx = pltpu.make_async_remote_copy(
        src_ref=stat_buf.at[0], dst_ref=stat_buf.at[1],
        send_sem=s_send, recv_sem=s_recv,
        device_id={"tp": other}, device_id_type=MESH)
    sx.start()

    for q in range(groups):
        each(q, lambda q, r, i: give_back(q, r, i).wait_send())
    sx.wait()
    total = squared + stat_buf[1][:, 0:1]
    scale = lax.rsqrt(total / features + RMS_EPS)
    out_ref[...] = (low * scale * post_ref[...]).astype(BF16)


def shards(n, n_tp, tokens, norm_gain, expert_ids, gates, w_gate, w_up, w_down, post_gain):
    rows, features = tokens.shape
    half = features // n_tp
    part = w_gate.shape[2]
    vmem = pl.BlockSpec(memory_space=pltpu.VMEM)
    hbm = pl.BlockSpec(memory_space=pl.ANY)
    dma = pltpu.SemaphoreType.DMA
    cap = n * SLOTS
    return pl.pallas_call(
        functools.partial(kernel, n, n_tp),
        out_shape=jax.ShapeDtypeStruct((rows, half), BF16),
        in_specs=[vmem] * 5 + [hbm] * 3,
        out_specs=vmem,
        scratch_shapes=[
            pltpu.VMEM((n, SLOTS, half), BF16),
            pltpu.VMEM((n, n_tp, SLOTS, half), BF16),
            pltpu.VMEM((features, 2 * part), BF16),
            pltpu.VMEM((n_tp * part, half), BF16),
            pltpu.VMEM((cap, n_tp * part), BF16),
            pltpu.VMEM((n, SLOTS, half), BF16),
            pltpu.VMEM((n, SLOTS, half), BF16),
            pltpu.VMEM((2, rows, 128), F32),
            dma((5,)), dma, dma,
            dma((n,)), dma((n,)), dma((n,)), dma((n,)),
            dma((2,)), dma((2,)), dma((n,)), dma((n,)), dma, dma,
        ],
        compiler_params=pltpu.CompilerParams(
            collective_id=0, has_side_effects=True, vmem_limit_bytes=60 * 1024 * 1024
        ),
    )(
        tokens, norm_gain.reshape(1, -1), expert_ids.T, gates.T, post_gain.reshape(1, -1),
        w_gate, w_up, w_down,
    )


def solution(mesh):
    in_specs = (
        P("ep", None),
        P(),
        P("ep", None),
        P("ep", None),
        P("ep", None, "tp"),
        P("ep", None, "tp"),
        P("ep", "tp", None),
        P("tp"),
    )
    body = functools.partial(shards, mesh.shape["ep"], mesh.shape["tp"])
    return jax.shard_map(body, mesh=mesh, in_specs=in_specs, out_specs=P("ep", "tp"), check_vma=False)
```

```python
import functools

import jax
import jax.numpy as jnp
from jax import lax
from jax.experimental import pallas as pl
from jax.experimental.pallas import tpu as pltpu
from jax.sharding import PartitionSpec as P

SLOTS = 8
RMS_EPS = 1e-06
MESH = pl.DeviceIdType.MESH
F32 = jnp.float32
BF16 = jnp.bfloat16


def kernel(
    n, n_tp,
    tok_ref, gain_ref, ids_ref, gates_ref, post_ref, wg_ref, wu_ref, wd_ref,
    out_ref,
    send_buf, x_buf, wgu, wdn, h_buf, o_buf, ret_buf, stat_buf,
    w_sem, wx_send, wx_recv, d_send, d_recv, f_send, f_recv,
    h_send, h_recv, r_send, r_recv, s_send, s_recv,
):
    me = lax.axis_index("ep")
    core = lax.axis_index("tp")
    other = 1 - core
    rows, features = tok_ref.shape
    half = features // n_tp
    part = wg_ref.shape[2]
    cap = n * SLOTS

    groups = 4 if n % 4 == 0 else 1
    order = (2, 1, 3, 0) if groups == 4 else (0,)
    wide = n // groups
    plane, place = me // wide, lax.rem(me, wide)

    def facing(code):
        pair = plane + 1 - 2 * lax.rem(plane, 2)
        return {0: plane, 1: pair, 2: lax.rem(plane + 2, 4), 3: 3 - plane}[code]

    def target(q, r):
        return facing(order[q]) * wide + lax.rem(place + r, wide)

    def origin(q, r):
        return facing(order[q]) * wide + lax.rem(place + wide - r, wide)

    def each(q, body):
        def go(r, _):
            body(q, r, q * wide + r)
            return 0

        lax.fori_loop(0 if order[q] else 1, wide, go, 0)

    own = order.index(0) * wide

    barrier = pltpu.get_barrier_semaphore()

    def greet(k, _):
        pl.semaphore_signal(barrier, inc=1, device_id={"ep": lax.rem(me + k, n)}, device_id_type=MESH)
        return 0

    lax.fori_loop(1, n, greet, 0)
    pl.semaphore_signal(barrier, inc=1, device_id={"tp": other}, device_id_type=MESH)

    own_cols = pl.ds(pl.multiple_of(core * half, half), half)
    other_cols = pl.ds(pl.multiple_of(other * half, half), half)
    own_part = pl.ds(pl.multiple_of(core * part, part), part)
    copies = [
        pltpu.make_async_copy(wg_ref.at[0], wgu.at[:, pl.ds(0, part)], w_sem.at[0]),
        pltpu.make_async_copy(wu_ref.at[0], wgu.at[:, pl.ds(part, part)], w_sem.at[1]),
        pltpu.make_async_copy(wd_ref.at[0, :, own_cols], wdn.at[own_part], w_sem.at[2]),
    ]
    for copy in copies:
        copy.start()

    ids = ids_ref[...]
    names = lax.broadcasted_iota(jnp.int32, (n, rows), 0)
    first = lax.broadcasted_iota(jnp.int32, (rows, rows), 0)
    second = lax.broadcasted_iota(jnp.int32, (rows, rows), 1)
    before = (first < second).astype(BF16)
    same = first == second
    slots = lax.broadcasted_iota(jnp.int32, (cap, rows), 0)
    count = jnp.zeros((n, 1), F32)
    picks = []
    for j in range(ids.shape[0]):
        hot = (ids[j:j + 1] == names).astype(F32)
        earlier = jnp.dot(hot.astype(BF16), before, preferred_element_type=F32) + count
        slot = jnp.sum(earlier * hot, axis=0, keepdims=True).astype(jnp.int32)
        count = count + jnp.sum(hot, axis=1, keepdims=True)
        picks.append((slots == ids[j:j + 1] * SLOTS + slot).astype(F32))

    floats = tok_ref[...].astype(F32)
    inverse = lax.rsqrt(jnp.mean(floats * floats, axis=1, keepdims=True) + RMS_EPS)
    mine = tok_ref[:, own_cols].astype(F32)
    normed = (mine * inverse * gain_ref[:, own_cols]).astype(BF16)
    dispatch = functools.reduce(lambda a, b: a + b, picks).astype(BF16)
    sent = jnp.dot(dispatch, normed, preferred_element_type=F32)
    send_buf[...] = sent.reshape(n, SLOTS, half).astype(BF16)

    pl.semaphore_wait(barrier, n)

    def to_expert(q, r, i):
        peer = target(q, r)
        return pltpu.make_async_remote_copy(
            src_ref=send_buf.at[peer], dst_ref=x_buf.at[i, core],
            send_sem=d_send.at[i], recv_sem=d_recv.at[i],
            device_id={"ep": peer}, device_id_type=MESH)

    def forward(src, block):
        return pltpu.make_async_remote_copy(
            src_ref=src, dst_ref=x_buf.at[block, core],
            send_sem=f_send.at[block], recv_sem=f_recv.at[block],
            device_id={"tp": other}, device_id_type=MESH)

    for q in range(groups):
        each(q, lambda q, r, i: to_expert(q, r, i).start())
    own_x = pltpu.make_async_copy(send_buf.at[me], x_buf.at[own, core], w_sem.at[3])
    own_x.start()
    forward(send_buf.at[me], own).start()
    down_x = pltpu.make_async_remote_copy(
        src_ref=wd_ref.at[0, :, other_cols], dst_ref=wdn.at[own_part],
        send_sem=wx_send, recv_sem=wx_recv,
        device_id={"tp": other}, device_id_type=MESH)
    down_x.start()
    own_r = pltpu.make_async_copy(o_buf.at[own], ret_buf.at[me], w_sem.at[4])

    def pass_on(q, r, i):
        to_expert(q, r, i).wait_recv()
        forward(x_buf.at[i, core], i).start()

    def give_back(q, r, i):
        peer = origin(q, r)
        return pltpu.make_async_remote_copy(
            src_ref=o_buf.at[i], dst_ref=ret_buf.at[me],
            send_sem=r_send.at[i], recv_sem=r_recv.at[me],
            device_id={"ep": peer}, device_id_type=MESH)

    def take_back(q, r, i):
        peer = target(q, r)
        return pltpu.make_async_remote_copy(
            src_ref=o_buf.at[i], dst_ref=ret_buf.at[peer],
            send_sem=r_send.at[i], recv_sem=r_recv.at[peer],
            device_id={"ep": peer}, device_id_type=MESH)

    span = max(groups // 2, 1)
    for chunk in range(groups // span):
        mine_q = range(chunk * span, (chunk + 1) * span)
        start, size = chunk * span * wide, span * wide
        for q in mine_q:
            each(q, pass_on)
        if start <= own < start + size:
            own_x.wait()

        def arrived(i, _):
            forward(x_buf.at[i, core], i).wait_recv()
            return 0

        lax.fori_loop(start, start + size, arrived, 0)
        if chunk == 0:
            for copy in copies:
                copy.wait()
        acc = jnp.zeros((size * SLOTS, 2 * part), F32)
        for side in range(n_tp):
            x = x_buf[start:start + size, side].astype(F32).reshape(size * SLOTS, half).astype(BF16)
            acc = acc + jnp.dot(x, wgu[side * half:(side + 1) * half], preferred_element_type=F32)
        gate = acc[:, :part]
        up = acc[:, part:]
        hidden = (gate / (1.0 + jnp.exp(-gate)) * up).astype(BF16)
        lines = pl.ds(start * SLOTS, size * SLOTS)
        h_buf[lines, own_part] = hidden
        hx = pltpu.make_async_remote_copy(
            src_ref=h_buf.at[lines, own_part], dst_ref=h_buf.at[lines, own_part],
            send_sem=h_send.at[chunk], recv_sem=h_recv.at[chunk],
            device_id={"tp": other}, device_id_type=MESH)
        hx.start()
        if chunk == 0:
            down_x.wait()
        hx.wait()
        result = jnp.dot(h_buf[lines], wdn[...], preferred_element_type=F32)
        o_buf[start:start + size] = result.reshape(size, SLOTS, half).astype(BF16)
        for q in mine_q:
            each(q, lambda q, r, i: give_back(q, r, i).start())
        if start <= own < start + size:
            own_r.start()

    for q in range(groups):
        each(q, lambda q, r, i: to_expert(q, r, i).wait_send())

    def passed_all(i, _):
        forward(x_buf.at[i, core], i).wait_send()
        return 0

    lax.fori_loop(0, n, passed_all, 0)
    gates = [
        jnp.sum(jnp.where(same, gates_ref[j:j + 1], 0.0), axis=1, keepdims=True)
        for j in range(ids.shape[0])
    ]
    picks = [pick.T.astype(BF16) for pick in picks]
    for q in range(groups):
        each(q, lambda q, r, i: take_back(q, r, i).wait_recv())
    own_r.wait()

    returned = ret_buf[...].astype(F32).reshape(cap, half).astype(BF16)
    combined = jnp.zeros((rows, half), F32)
    for j, pick in enumerate(picks):
        row = jnp.dot(pick, returned, preferred_element_type=F32)
        combined = combined + gates[j] * row
    low = combined.astype(BF16).astype(F32)
    squared = jnp.sum(low * low, axis=1, keepdims=True)
    stat_buf[0] = jnp.broadcast_to(squared, (rows, 128))
    sx = pltpu.make_async_remote_copy(
        src_ref=stat_buf.at[0], dst_ref=stat_buf.at[1],
        send_sem=s_send, recv_sem=s_recv,
        device_id={"tp": other}, device_id_type=MESH)
    sx.start()

    for q in range(groups):
        each(q, lambda q, r, i: give_back(q, r, i).wait_send())
    sx.wait()
    total = squared + stat_buf[1][:, 0:1]
    scale = lax.rsqrt(total / features + RMS_EPS)
    out_ref[...] = (low * scale * post_ref[...]).astype(BF16)


def shards(n, n_tp, tokens, norm_gain, expert_ids, gates, w_gate, w_up, w_down, post_gain):
    rows, features = tokens.shape
    half = features // n_tp
    part = w_gate.shape[2]
    vmem = pl.BlockSpec(memory_space=pltpu.VMEM)
    hbm = pl.BlockSpec(memory_space=pl.ANY)
    dma = pltpu.SemaphoreType.DMA
    cap = n * SLOTS
    return pl.pallas_call(
        functools.partial(kernel, n, n_tp),
        out_shape=jax.ShapeDtypeStruct((rows, half), BF16),
        in_specs=[vmem] * 5 + [hbm] * 3,
        out_specs=vmem,
        scratch_shapes=[
            pltpu.VMEM((n, SLOTS, half), BF16),
            pltpu.VMEM((n, n_tp, SLOTS, half), BF16),
            pltpu.VMEM((features, 2 * part), BF16),
            pltpu.VMEM((n_tp * part, half), BF16),
            pltpu.VMEM((cap, n_tp * part), BF16),
            pltpu.VMEM((n, SLOTS, half), BF16),
            pltpu.VMEM((n, SLOTS, half), BF16),
            pltpu.VMEM((2, rows, 128), F32),
            dma((5,)), dma, dma,
            dma((n,)), dma((n,)), dma((n,)), dma((n,)),
            dma((2,)), dma((2,)), dma((n,)), dma((n,)), dma, dma,
        ],
        compiler_params=pltpu.CompilerParams(
            collective_id=0, has_side_effects=True, vmem_limit_bytes=60 * 1024 * 1024
        ),
    )(
        tokens, norm_gain.reshape(1, -1), expert_ids.T, gates.T, post_gain.reshape(1, -1),
        w_gate, w_up, w_down,
    )


def solution(mesh):
    in_specs = (
        P("ep", None),
        P(),
        P("ep", None),
        P("ep", None),
        P("ep", None, "tp"),
        P("ep", None, "tp"),
        P("ep", "tp", None),
        P("tp"),
    )
    body = functools.partial(shards, mesh.shape["ep"], mesh.shape["tp"])
    return jax.shard_map(body, mesh=mesh, in_specs=in_specs, out_specs=P("ep", "tp"), check_vma=False)
```

```python
import functools

import jax
import jax.numpy as jnp
from jax import lax
from jax.experimental import pallas as pl
from jax.experimental.pallas import tpu as pltpu
from jax.sharding import PartitionSpec as P

SLOTS = 8
RMS_EPS = 1e-06
MESH = pl.DeviceIdType.MESH
F32 = jnp.float32
BF16 = jnp.bfloat16


def kernel(
    n, n_tp,
    tok_ref, gain_ref, ids_ref, gates_ref, post_ref, wg_ref, wu_ref, wd_ref,
    out_ref,
    send_buf, x_buf, wgu, wdn, h_buf, o_buf, ret_buf, stat_buf,
    w_sem, wx_send, wx_recv, d_send, d_recv, f_send, f_recv,
    h_send, h_recv, r_send, r_recv, s_send, s_recv,
):
    me = lax.axis_index("ep")
    core = lax.axis_index("tp")
    other = 1 - core
    rows, features = tok_ref.shape
    half = features // n_tp
    part = wg_ref.shape[2]
    cap = n * SLOTS

    groups = 4 if n % 4 == 0 else 1
    order = (2, 1, 3, 0) if groups == 4 else (0,)
    wide = n // groups
    plane, place = me // wide, lax.rem(me, wide)

    def facing(code):
        pair = plane + 1 - 2 * lax.rem(plane, 2)
        return {0: plane, 1: pair, 2: lax.rem(plane + 2, 4), 3: 3 - plane}[code]

    def target(q, r):
        return facing(order[q]) * wide + lax.rem(place + r, wide)

    def origin(q, r):
        return facing(order[q]) * wide + lax.rem(place + wide - r, wide)

    def each(q, body):
        def go(r, _):
            body(q, r, q * wide + r)
            return 0

        lax.fori_loop(0 if order[q] else 1, wide, go, 0)

    own = order.index(0) * wide

    barrier = pltpu.get_barrier_semaphore()

    def greet(k, _):
        pl.semaphore_signal(barrier, inc=1, device_id={"ep": lax.rem(me + k, n)}, device_id_type=MESH)
        return 0

    lax.fori_loop(1, n, greet, 0)
    pl.semaphore_signal(barrier, inc=1, device_id={"tp": other}, device_id_type=MESH)

    own_cols = pl.ds(pl.multiple_of(core * half, half), half)
    other_cols = pl.ds(pl.multiple_of(other * half, half), half)
    own_part = pl.ds(pl.multiple_of(core * part, part), part)
    copies = [
        pltpu.make_async_copy(wg_ref.at[0], wgu.at[:, pl.ds(0, part)], w_sem.at[0]),
        pltpu.make_async_copy(wu_ref.at[0], wgu.at[:, pl.ds(part, part)], w_sem.at[1]),
        pltpu.make_async_copy(wd_ref.at[0, :, own_cols], wdn.at[own_part], w_sem.at[2]),
    ]
    for copy in copies:
        copy.start()

    ids = ids_ref[...]
    names = lax.broadcasted_iota(jnp.int32, (n, rows), 0)
    first = lax.broadcasted_iota(jnp.int32, (rows, rows), 0)
    second = lax.broadcasted_iota(jnp.int32, (rows, rows), 1)
    before = (first < second).astype(BF16)
    same = first == second
    slots = lax.broadcasted_iota(jnp.int32, (cap, rows), 0)
    count = jnp.zeros((n, 1), F32)
    picks = []
    for j in range(ids.shape[0]):
        hot = (ids[j:j + 1] == names).astype(F32)
        earlier = jnp.dot(hot.astype(BF16), before, preferred_element_type=F32) + count
        slot = jnp.sum(earlier * hot, axis=0, keepdims=True).astype(jnp.int32)
        count = count + jnp.sum(hot, axis=1, keepdims=True)
        picks.append((slots == ids[j:j + 1] * SLOTS + slot).astype(F32))

    floats = tok_ref[...].astype(F32)
    inverse = lax.rsqrt(jnp.mean(floats * floats, axis=1, keepdims=True) + RMS_EPS)
    mine = tok_ref[:, own_cols].astype(F32)
    normed = (mine * inverse * gain_ref[:, own_cols]).astype(BF16)
    dispatch = functools.reduce(lambda a, b: a + b, picks).astype(BF16)
    sent = jnp.dot(dispatch, normed, preferred_element_type=F32)
    send_buf[...] = sent.reshape(n, SLOTS, half).astype(BF16)

    pl.semaphore_wait(barrier, n)

    def to_expert(q, r, i):
        peer = target(q, r)
        return pltpu.make_async_remote_copy(
            src_ref=send_buf.at[peer], dst_ref=x_buf.at[i, core],
            send_sem=d_send.at[i], recv_sem=d_recv.at[i],
            device_id={"ep": peer}, device_id_type=MESH)

    def forward(src, block):
        return pltpu.make_async_remote_copy(
            src_ref=src, dst_ref=x_buf.at[block, core],
            send_sem=f_send.at[block], recv_sem=f_recv.at[block],
            device_id={"tp": other}, device_id_type=MESH)

    for q in (0, 1, 3) if groups == 4 else (0,):
        each(q, lambda q, r, i: to_expert(q, r, i).start())
    own_x = pltpu.make_async_copy(send_buf.at[me], x_buf.at[own, core], w_sem.at[3])
    own_x.start()
    forward(send_buf.at[me], own).start()
    down_x = pltpu.make_async_remote_copy(
        src_ref=wd_ref.at[0, :, other_cols], dst_ref=wdn.at[own_part],
        send_sem=wx_send, recv_sem=wx_recv,
        device_id={"tp": other}, device_id_type=MESH)
    down_x.start()
    own_r = pltpu.make_async_copy(o_buf.at[own], ret_buf.at[me], w_sem.at[4])

    def pass_on(q, r, i):
        to_expert(q, r, i).wait_recv()
        forward(x_buf.at[i, core], i).start()
        if groups == 4 and q == 0:
            to_expert(2, r, 2 * wide + r).start()

    def give_back(q, r, i):
        peer = origin(q, r)
        return pltpu.make_async_remote_copy(
            src_ref=o_buf.at[i], dst_ref=ret_buf.at[me],
            send_sem=r_send.at[i], recv_sem=r_recv.at[me],
            device_id={"ep": peer}, device_id_type=MESH)

    def take_back(q, r, i):
        peer = target(q, r)
        return pltpu.make_async_remote_copy(
            src_ref=o_buf.at[i], dst_ref=ret_buf.at[peer],
            send_sem=r_send.at[i], recv_sem=r_recv.at[peer],
            device_id={"ep": peer}, device_id_type=MESH)

    span = max(groups // 2, 1)
    for chunk in range(groups // span):
        mine_q = range(chunk * span, (chunk + 1) * span)
        start, size = chunk * span * wide, span * wide
        for q in mine_q:
            each(q, pass_on)
        if start <= own < start + size:
            own_x.wait()

        def arrived(i, _):
            forward(x_buf.at[i, core], i).wait_recv()
            return 0

        lax.fori_loop(start, start + size, arrived, 0)
        if chunk == 0:
            for copy in copies:
                copy.wait()
        acc = jnp.zeros((size * SLOTS, 2 * part), F32)
        for side in range(n_tp):
            x = x_buf[start:start + size, side].astype(F32).reshape(size * SLOTS, half).astype(BF16)
            acc = acc + jnp.dot(x, wgu[side * half:(side + 1) * half], preferred_element_type=F32)
        gate = acc[:, :part]
        up = acc[:, part:]
        hidden = (gate / (1.0 + jnp.exp(-gate)) * up).astype(BF16)
        lines = pl.ds(start * SLOTS, size * SLOTS)
        h_buf[lines, own_part] = hidden
        hx = pltpu.make_async_remote_copy(
            src_ref=h_buf.at[lines, own_part], dst_ref=h_buf.at[lines, own_part],
            send_sem=h_send.at[chunk], recv_sem=h_recv.at[chunk],
            device_id={"tp": other}, device_id_type=MESH)
        hx.start()
        if chunk == 0:
            down_x.wait()
        hx.wait()
        result = jnp.dot(h_buf[lines], wdn[...], preferred_element_type=F32)
        o_buf[start:start + size] = result.reshape(size, SLOTS, half).astype(BF16)
        for q in mine_q:
            each(q, lambda q, r, i: give_back(q, r, i).start())
        if start <= own < start + size:
            own_r.start()

    for q in range(groups):
        each(q, lambda q, r, i: to_expert(q, r, i).wait_send())

    def passed_all(i, _):
        forward(x_buf.at[i, core], i).wait_send()
        return 0

    lax.fori_loop(0, n, passed_all, 0)
    gates = [
        jnp.sum(jnp.where(same, gates_ref[j:j + 1], 0.0), axis=1, keepdims=True)
        for j in range(ids.shape[0])
    ]
    picks = [pick.T.astype(BF16) for pick in picks]
    for q in range(groups):
        each(q, lambda q, r, i: take_back(q, r, i).wait_recv())
    own_r.wait()

    returned = ret_buf[...].astype(F32).reshape(cap, half).astype(BF16)
    combined = jnp.zeros((rows, half), F32)
    for j, pick in enumerate(picks):
        row = jnp.dot(pick, returned, preferred_element_type=F32)
        combined = combined + gates[j] * row
    low = combined.astype(BF16).astype(F32)
    squared = jnp.sum(low * low, axis=1, keepdims=True)
    stat_buf[0] = jnp.broadcast_to(squared, (rows, 128))
    sx = pltpu.make_async_remote_copy(
        src_ref=stat_buf.at[0], dst_ref=stat_buf.at[1],
        send_sem=s_send, recv_sem=s_recv,
        device_id={"tp": other}, device_id_type=MESH)
    sx.start()

    for q in range(groups):
        each(q, lambda q, r, i: give_back(q, r, i).wait_send())
    sx.wait()
    total = squared + stat_buf[1][:, 0:1]
    scale = lax.rsqrt(total / features + RMS_EPS)
    out_ref[...] = (low * scale * post_ref[...]).astype(BF16)


def shards(n, n_tp, tokens, norm_gain, expert_ids, gates, w_gate, w_up, w_down, post_gain):
    rows, features = tokens.shape
    half = features // n_tp
    part = w_gate.shape[2]
    vmem = pl.BlockSpec(memory_space=pltpu.VMEM)
    hbm = pl.BlockSpec(memory_space=pl.ANY)
    dma = pltpu.SemaphoreType.DMA
    cap = n * SLOTS
    return pl.pallas_call(
        functools.partial(kernel, n, n_tp),
        out_shape=jax.ShapeDtypeStruct((rows, half), BF16),
        in_specs=[vmem] * 5 + [hbm] * 3,
        out_specs=vmem,
        scratch_shapes=[
            pltpu.VMEM((n, SLOTS, half), BF16),
            pltpu.VMEM((n, n_tp, SLOTS, half), BF16),
            pltpu.VMEM((features, 2 * part), BF16),
            pltpu.VMEM((n_tp * part, half), BF16),
            pltpu.VMEM((cap, n_tp * part), BF16),
            pltpu.VMEM((n, SLOTS, half), BF16),
            pltpu.VMEM((n, SLOTS, half), BF16),
            pltpu.VMEM((2, rows, 128), F32),
            dma((5,)), dma, dma,
            dma((n,)), dma((n,)), dma((n,)), dma((n,)),
            dma((2,)), dma((2,)), dma((n,)), dma((n,)), dma, dma,
        ],
        compiler_params=pltpu.CompilerParams(
            collective_id=0, has_side_effects=True, vmem_limit_bytes=60 * 1024 * 1024
        ),
    )(
        tokens, norm_gain.reshape(1, -1), expert_ids.T, gates.T, post_gain.reshape(1, -1),
        w_gate, w_up, w_down,
    )


def solution(mesh):
    in_specs = (
        P("ep", None),
        P(),
        P("ep", None),
        P("ep", None),
        P("ep", None, "tp"),
        P("ep", None, "tp"),
        P("ep", "tp", None),
        P("tp"),
    )
    body = functools.partial(shards, mesh.shape["ep"], mesh.shape["tp"])
    return jax.shard_map(body, mesh=mesh, in_specs=in_specs, out_specs=P("ep", "tp"), check_vma=False)
```

```python
import functools

import jax
import jax.numpy as jnp
from jax import lax
from jax.experimental import pallas as pl
from jax.experimental.pallas import tpu as pltpu
from jax.sharding import PartitionSpec as P

SLOTS = 8
RMS_EPS = 1e-06
MESH = pl.DeviceIdType.MESH
F32 = jnp.float32
BF16 = jnp.bfloat16


def kernel(
    n, n_tp,
    tok_ref, gain_ref, ids_ref, gates_ref, post_ref, wg_ref, wu_ref, wd_ref,
    out_ref,
    send_buf, x_buf, wgu, wdn, h_buf, o_buf, ret_buf, stat_buf,
    w_sem, wx_send, wx_recv, d_send, d_recv, f_send, f_recv,
    h_send, h_recv, r_send, r_recv, s_send, s_recv,
):
    me = lax.axis_index("ep")
    core = lax.axis_index("tp")
    other = 1 - core
    rows, features = tok_ref.shape
    half = features // n_tp
    part = wg_ref.shape[2]
    cap = n * SLOTS

    groups = 4 if n % 4 == 0 else 1
    order = (2, 1, 3, 0) if groups == 4 else (0,)
    wide = n // groups
    plane, place = me // wide, lax.rem(me, wide)

    def facing(code):
        pair = plane + 1 - 2 * lax.rem(plane, 2)
        return {0: plane, 1: pair, 2: lax.rem(plane + 2, 4), 3: 3 - plane}[code]

    def target(q, r):
        return facing(order[q]) * wide + lax.rem(place + r, wide)

    def origin(q, r):
        return facing(order[q]) * wide + lax.rem(place + wide - r, wide)

    def each(q, body):
        def go(r, _):
            r = (wide - 1 if order[q] else wide) - r
            body(q, r, q * wide + r)
            return 0

        lax.fori_loop(0 if order[q] else 1, wide, go, 0)

    own = order.index(0) * wide

    barrier = pltpu.get_barrier_semaphore()

    def greet(k, _):
        pl.semaphore_signal(barrier, inc=1, device_id={"ep": lax.rem(me + k, n)}, device_id_type=MESH)
        return 0

    lax.fori_loop(1, n, greet, 0)
    pl.semaphore_signal(barrier, inc=1, device_id={"tp": other}, device_id_type=MESH)

    own_cols = pl.ds(pl.multiple_of(core * half, half), half)
    other_cols = pl.ds(pl.multiple_of(other * half, half), half)
    own_part = pl.ds(pl.multiple_of(core * part, part), part)
    copies = [
        pltpu.make_async_copy(wg_ref.at[0], wgu.at[:, pl.ds(0, part)], w_sem.at[0]),
        pltpu.make_async_copy(wu_ref.at[0], wgu.at[:, pl.ds(part, part)], w_sem.at[1]),
        pltpu.make_async_copy(wd_ref.at[0, :, own_cols], wdn.at[own_part], w_sem.at[2]),
    ]
    for copy in copies:
        copy.start()

    ids = ids_ref[...]
    names = lax.broadcasted_iota(jnp.int32, (n, rows), 0)
    first = lax.broadcasted_iota(jnp.int32, (rows, rows), 0)
    second = lax.broadcasted_iota(jnp.int32, (rows, rows), 1)
    before = (first < second).astype(BF16)
    same = first == second
    slots = lax.broadcasted_iota(jnp.int32, (cap, rows), 0)
    count = jnp.zeros((n, 1), F32)
    picks = []
    for j in range(ids.shape[0]):
        hot = (ids[j:j + 1] == names).astype(F32)
        earlier = jnp.dot(hot.astype(BF16), before, preferred_element_type=F32) + count
        slot = jnp.sum(earlier * hot, axis=0, keepdims=True).astype(jnp.int32)
        count = count + jnp.sum(hot, axis=1, keepdims=True)
        picks.append((slots == ids[j:j + 1] * SLOTS + slot).astype(F32))

    floats = tok_ref[...].astype(F32)
    inverse = lax.rsqrt(jnp.mean(floats * floats, axis=1, keepdims=True) + RMS_EPS)
    mine = tok_ref[:, own_cols].astype(F32)
    normed = (mine * inverse * gain_ref[:, own_cols]).astype(BF16)
    dispatch = functools.reduce(lambda a, b: a + b, picks).astype(BF16)
    sent = jnp.dot(dispatch, normed, preferred_element_type=F32)
    send_buf[...] = sent.reshape(n, SLOTS, half).astype(BF16)

    pl.semaphore_wait(barrier, n)

    def to_expert(q, r, i):
        peer = target(q, r)
        return pltpu.make_async_remote_copy(
            src_ref=send_buf.at[peer], dst_ref=x_buf.at[i, core],
            send_sem=d_send.at[i], recv_sem=d_recv.at[i],
            device_id={"ep": peer}, device_id_type=MESH)

    def forward(src, block):
        return pltpu.make_async_remote_copy(
            src_ref=src, dst_ref=x_buf.at[block, core],
            send_sem=f_send.at[block], recv_sem=f_recv.at[block],
            device_id={"tp": other}, device_id_type=MESH)

    for q in (0, 1, 3) if groups == 4 else (0,):
        each(q, lambda q, r, i: to_expert(q, r, i).start())
    own_x = pltpu.make_async_copy(send_buf.at[me], x_buf.at[own, core], w_sem.at[3])
    own_x.start()
    forward(send_buf.at[me], own).start()
    down_x = pltpu.make_async_remote_copy(
        src_ref=wd_ref.at[0, :, other_cols], dst_ref=wdn.at[own_part],
        send_sem=wx_send, recv_sem=wx_recv,
        device_id={"tp": other}, device_id_type=MESH)
    down_x.start()
    own_r = pltpu.make_async_copy(o_buf.at[own], ret_buf.at[me], w_sem.at[4])

    def pass_on(q, r, i):
        to_expert(q, r, i).wait_recv()
        forward(x_buf.at[i, core], i).start()
        if groups == 4 and q == 0:
            to_expert(2, r, 2 * wide + r).start()

    def give_back(q, r, i):
        peer = origin(q, r)
        return pltpu.make_async_remote_copy(
            src_ref=o_buf.at[i], dst_ref=ret_buf.at[me],
            send_sem=r_send.at[i], recv_sem=r_recv.at[me],
            device_id={"ep": peer}, device_id_type=MESH)

    def take_back(q, r, i):
        peer = target(q, r)
        return pltpu.make_async_remote_copy(
            src_ref=o_buf.at[i], dst_ref=ret_buf.at[peer],
            send_sem=r_send.at[i], recv_sem=r_recv.at[peer],
            device_id={"ep": peer}, device_id_type=MESH)

    span = max(groups // 2, 1)
    for chunk in range(groups // span):
        mine_q = range(chunk * span, (chunk + 1) * span)
        start, size = chunk * span * wide, span * wide
        for q in mine_q:
            each(q, pass_on)
        if start <= own < start + size:
            own_x.wait()

        def arrived(i, _):
            forward(x_buf.at[i, core], i).wait_recv()
            return 0

        lax.fori_loop(start, start + size, arrived, 0)
        if chunk == 0:
            for copy in copies:
                copy.wait()
        acc = jnp.zeros((size * SLOTS, 2 * part), F32)
        for side in range(n_tp):
            x = x_buf[start:start + size, side].astype(F32).reshape(size * SLOTS, half).astype(BF16)
            acc = acc + jnp.dot(x, wgu[side * half:(side + 1) * half], preferred_element_type=F32)
        gate = acc[:, :part]
        up = acc[:, part:]
        hidden = (gate / (1.0 + jnp.exp(-gate)) * up).astype(BF16)
        lines = pl.ds(start * SLOTS, size * SLOTS)
        h_buf[lines, own_part] = hidden
        hx = pltpu.make_async_remote_copy(
            src_ref=h_buf.at[lines, own_part], dst_ref=h_buf.at[lines, own_part],
            send_sem=h_send.at[chunk], recv_sem=h_recv.at[chunk],
            device_id={"tp": other}, device_id_type=MESH)
        hx.start()
        if chunk == 0:
            down_x.wait()
        hx.wait()
        result = jnp.dot(h_buf[lines], wdn[...], preferred_element_type=F32)
        o_buf[start:start + size] = result.reshape(size, SLOTS, half).astype(BF16)
        for q in mine_q:
            each(q, lambda q, r, i: give_back(q, r, i).start())
        if start <= own < start + size:
            own_r.start()

    for q in range(groups):
        each(q, lambda q, r, i: to_expert(q, r, i).wait_send())

    def passed_all(i, _):
        forward(x_buf.at[i, core], i).wait_send()
        return 0

    lax.fori_loop(0, n, passed_all, 0)
    gates = [
        jnp.sum(jnp.where(same, gates_ref[j:j + 1], 0.0), axis=1, keepdims=True)
        for j in range(ids.shape[0])
    ]
    picks = [pick.T.astype(BF16) for pick in picks]
    for q in range(groups):
        each(q, lambda q, r, i: take_back(q, r, i).wait_recv())
    own_r.wait()

    returned = ret_buf[...].astype(F32).reshape(cap, half).astype(BF16)
    combined = jnp.zeros((rows, half), F32)
    for j, pick in enumerate(picks):
        row = jnp.dot(pick, returned, preferred_element_type=F32)
        combined = combined + gates[j] * row
    low = combined.astype(BF16).astype(F32)
    squared = jnp.sum(low * low, axis=1, keepdims=True)
    stat_buf[0] = jnp.broadcast_to(squared, (rows, 128))
    sx = pltpu.make_async_remote_copy(
        src_ref=stat_buf.at[0], dst_ref=stat_buf.at[1],
        send_sem=s_send, recv_sem=s_recv,
        device_id={"tp": other}, device_id_type=MESH)
    sx.start()

    for q in range(groups):
        each(q, lambda q, r, i: give_back(q, r, i).wait_send())
    sx.wait()
    total = squared + stat_buf[1][:, 0:1]
    scale = lax.rsqrt(total / features + RMS_EPS)
    out_ref[...] = (low * scale * post_ref[...]).astype(BF16)


def shards(n, n_tp, tokens, norm_gain, expert_ids, gates, w_gate, w_up, w_down, post_gain):
    rows, features = tokens.shape
    half = features // n_tp
    part = w_gate.shape[2]
    vmem = pl.BlockSpec(memory_space=pltpu.VMEM)
    hbm = pl.BlockSpec(memory_space=pl.ANY)
    dma = pltpu.SemaphoreType.DMA
    cap = n * SLOTS
    return pl.pallas_call(
        functools.partial(kernel, n, n_tp),
        out_shape=jax.ShapeDtypeStruct((rows, half), BF16),
        in_specs=[vmem] * 5 + [hbm] * 3,
        out_specs=vmem,
        scratch_shapes=[
            pltpu.VMEM((n, SLOTS, half), BF16),
            pltpu.VMEM((n, n_tp, SLOTS, half), BF16),
            pltpu.VMEM((features, 2 * part), BF16),
            pltpu.VMEM((n_tp * part, half), BF16),
            pltpu.VMEM((cap, n_tp * part), BF16),
            pltpu.VMEM((n, SLOTS, half), BF16),
            pltpu.VMEM((n, SLOTS, half), BF16),
            pltpu.VMEM((2, rows, 128), F32),
            dma((5,)), dma, dma,
            dma((n,)), dma((n,)), dma((n,)), dma((n,)),
            dma((2,)), dma((2,)), dma((n,)), dma((n,)), dma, dma,
        ],
        compiler_params=pltpu.CompilerParams(
            collective_id=0, has_side_effects=True, vmem_limit_bytes=60 * 1024 * 1024
        ),
    )(
        tokens, norm_gain.reshape(1, -1), expert_ids.T, gates.T, post_gain.reshape(1, -1),
        w_gate, w_up, w_down,
    )


def solution(mesh):
    in_specs = (
        P("ep", None),
        P(),
        P("ep", None),
        P("ep", None),
        P("ep", None, "tp"),
        P("ep", None, "tp"),
        P("ep", "tp", None),
        P("tp"),
    )
    body = functools.partial(shards, mesh.shape["ep"], mesh.shape["tp"])
    return jax.shard_map(body, mesh=mesh, in_specs=in_specs, out_specs=P("ep", "tp"), check_vma=False)
```
